32 devices in a mesh: sp: 32 (over z, y, x, core), fs: 1, tp: 1.
Axes of the slice: x: 2, y: 2, z: 4, core: 2. Of those that a mesh axis runs over, the one named last changes fastest.
Arguments:
- tokens: bfloat16 [4096, 2048], P(('fs', 'sp'), 'tp'), may hold values from -450 to 450
- documents: int32 [4096], P(('fs', 'sp')), may hold values from 0 to 3, never falling along the last dimension, each value on 1 to 2048 neighbouring positions
- norm_gain: bfloat16 [2048], P('tp'), may hold values from 0.099609375 to 1.8984375
- out_gate_weight: bfloat16 [2048, 1024], P('sp', 'tp'), may hold values from -0.125 to 0.125
- in_gate_weight: bfloat16 [2048, 1024], P('sp', 'tp'), may hold values from -0.125 to 0.125
- value_weight: bfloat16 [2048, 1024], P('sp', 'tp'), may hold values from -0.125 to 0.125
- conv_taps: bfloat16 [3, 1024], P(None, 'tp'), may hold values from -3.5 to 3.5
- state_in_weight: bfloat16 [2048, 1024], P('sp', 'tp'), may hold values from -0.125 to 0.125
- decay_rate: float32 [64, 64], P('tp'), may hold values from 4e-05 to 2.01
- frequency: float32 [64, 64], P('tp'), may hold values from 0 to 32
- step_log: float32 [64], P('tp'), may hold values from -3.9121 to -1.6094
- input_real: float32 [64, 64, 16], P('tp'), may hold values from -1 to 1
- input_imag: float32 [64, 64, 16], P('tp'), may hold values from -1 to 1
- readout_real: float32 [64, 16, 64], P('tp'), may hold values from -0.75 to 0.75
- readout_imag: float32 [64, 16, 64], P('tp'), may hold values from -0.75 to 0.75
- skip_gain: float32 [1024], P('tp'), may hold values from -4 to 4
- conv_out_weight: bfloat16 [1024, 2048], P('tp', 'sp'), may hold values from -0.125 to 0.125
- state_out_weight: bfloat16 [1024, 2048], P('tp', 'sp'), may hold values from -0.125 to 0.125
Outputs:
- mixed: bfloat16 [4096, 2048], P(('fs', 'sp', 'tp'))
The draws below stay inside these ranges and needn't reach their ends.
All inputs are finite; a program needn't handle non-finite values.
Results may differ from the reference program's by a relative error of at most 0.015.
Values may be sent and summed in bfloat16 or wider, within the bound.
No kernel may reach another device: no remote copies, remote signals or barrier semaphores. Data moves between devices by JAX's collectives and lax.ppermute only.
A program may use at most 64 MiB of HBM per device.

```python
import math
import jax
import jax.numpy as jnp
import numpy as np
from jax import lax

D = 2048
CONV = 1024
SSM = 1024
GROUP = 16
STATE = 64
TAPS = 3
BLOCK = 64
TOKENS = 4096
GROUPS = 64
DOCS = 4
DOC_MOST = 2048
N_TP = 1


def draw_tokens(key, part):
    streams = jax.random.split(jax.random.fold_in(key, 11), 4)
    noise = jnp.clip(jax.random.normal(streams[0], (TOKENS, D), jnp.float32), -5.0, 5.0)
    row_scale = jnp.exp(jax.random.uniform(streams[1], (TOKENS, 1), jnp.float32, 0.0, math.log(10.0)))
    col_scale = jnp.exp(jax.random.uniform(streams[2], (1, D), jnp.float32, 0.0, math.log(3.0)))
    upper_half = jnp.arange(D) >= D // 2
    swapped = jax.random.bernoulli(streams[3])
    half_scale = jnp.where(jnp.logical_xor(upper_half, swapped), 3.0, 1.0)
    return (noise * row_scale * col_scale * half_scale[None, :]).astype(jnp.bfloat16)


def rate_table(key):
    streams = jax.random.split(jax.random.fold_in(key, 23), 4)
    step_log = jax.random.uniform(streams[0], (GROUPS,), jnp.float32, math.log(0.02), math.log(0.2))
    share = 0.5
    slow_mask = jax.random.uniform(streams[1], (GROUPS, 1), jnp.float32) < share
    slow_part = jnp.exp(jax.random.uniform(streams[2], (GROUPS, STATE), jnp.float32, math.log(1e-05), math.log(5e-05)))
    fast_part = jnp.exp(jax.random.uniform(streams[3], (GROUPS, STATE), jnp.float32, math.log(0.02), math.log(0.04)))
    product = jnp.where(slow_mask, slow_part, fast_part)
    return (step_log, product / jnp.exp(step_log)[:, None])


def draw_step_log(key, part):
    return rate_table(key)[0]


def draw_decay_rate(key, part):
    return rate_table(key)[1]


def block_levels(key, dims, cuts, low, high):
    loudness, own = 1.0, jax.random.fold_in(key, 6)
    for position, parts in cuts:
        draws = jnp.exp(jax.random.uniform(jax.random.fold_in(own, position), (parts,), jnp.float32, low / len(cuts), high / len(cuts)))
        loudness = loudness * jnp.repeat(draws, dims[position] // parts).reshape([-1 if axis == position else 1 for axis in range(len(dims))])
    return loudness


def split_up(count, total, most, lean):
    loads = [(1 << 20) // math.isqrt(rank ** lean) + 1 for rank in range(2, count + 1)]
    surplus, given = total - most - (count - 1), [1] * (count - 1)
    while surplus > 0:
        candidates = [i for i in range(count - 1) if given[i] < most]
        whole, remaining = sum([loads[i] for i in candidates]), surplus
        for i in candidates:
            more = min(most - given[i], max(1, remaining * loads[i] // whole), surplus)
            given[i] = given[i] + more
            surplus = surplus - more
    return np.array([most] + given)


def uneven(rng, number_of, total, bound, lean):
    if number_of == 2:
        one = jax.random.randint(rng, (), max(1, total - bound), min(bound, total - 1) + 1)
        return jnp.stack([one, total - one])
    tallies = jnp.asarray(split_up(number_of, total, bound, lean), jnp.int32)
    pairs = (number_of - 1) // 2
    giver, receiver = tallies[1:1 + 2 * pairs:2], tallies[2:2 + 2 * pairs:2]
    room = jnp.minimum(giver - 1, bound - receiver)
    passed = jax.random.randint(jax.random.fold_in(rng, 1), (pairs,), 0, 1 << 20) % (room + 1)
    tallies = tallies.at[1:1 + 2 * pairs:2].set(giver - passed).at[2:2 + 2 * pairs:2].set(receiver + passed)
    return tallies[jax.random.permutation(jax.random.fold_in(rng, 2), number_of)]


def bell_draw(stream_key, shape, deviation, reach, cuts=(), held_as=jnp.bfloat16):
    values = deviation * jax.random.normal(stream_key, shape, jnp.float32)
    if cuts:
        values = values * block_levels(stream_key, shape, cuts, -0.22, 0.18)
    return jnp.clip(values, -reach, reach).astype(held_as)


def setup_inputs(seed: int = 0, part: int = 0) -> dict:
    key_list = jax.random.split(jax.random.key(seed), 19)
    part_keys = jax.random.split(jax.random.fold_in(key_list[18], part), 19)
    tokens = draw_tokens(jax.random.fold_in(jax.random.fold_in(key_list[18], part), 71), part)
    documents = jnp.searchsorted(jnp.cumsum(uneven(part_keys[1], DOCS, TOKENS, DOC_MOST, 0)), jnp.arange(TOKENS), side="right").astype(jnp.int32)
    norm_gain = jnp.clip(1.0 + 0.18 * jax.random.normal(key_list[2], (D,), jnp.float32), 0.099609375, 1.8984375).astype(jnp.bfloat16)
    out_gate_weight = bell_draw(key_list[3], (D, CONV), D ** -0.5, 0.125, ((0, 32),))
    in_gate_weight = bell_draw(key_list[4], (D, CONV), D ** -0.5, 0.125, ((0, 32),))
    value_weight = bell_draw(key_list[5], (D, CONV), D ** -0.5, 0.125, ((0, 32),))
    conv_taps = bell_draw(key_list[6], (TAPS, CONV), TAPS ** -0.5, 3.5)
    state_in_weight = bell_draw(key_list[7], (D, SSM), D ** -0.5, 0.125, ((0, 32),))
    decay_rate = draw_decay_rate(jax.random.fold_in(key_list[18], 71), part)
    frequency = jnp.clip(jax.random.uniform(key_list[9], (GROUPS, STATE), jnp.float32, 0.0, 32.0), 0.0, 32.0)
    step_log = draw_step_log(jax.random.fold_in(key_list[18], 71), part)
    input_real = bell_draw(key_list[11], (GROUPS, STATE, GROUP), (2 * GROUP) ** -0.5, 1.0, (), jnp.float32)
    input_imag = bell_draw(key_list[12], (GROUPS, STATE, GROUP), (2 * GROUP) ** -0.5, 1.0, (), jnp.float32)
    readout_real = bell_draw(key_list[13], (GROUPS, GROUP, STATE), STATE ** -0.5, 0.75, (), jnp.float32)
    readout_imag = bell_draw(key_list[14], (GROUPS, GROUP, STATE), STATE ** -0.5, 0.75, (), jnp.float32)
    skip_gain = bell_draw(key_list[15], (SSM,), 1.0, 4.0, (), jnp.float32)
    conv_out_weight = bell_draw(key_list[16], (CONV, D), (CONV + SSM) ** -0.5, 0.125, ((1, 32),))
    state_out_weight = bell_draw(key_list[17], (SSM, D), (CONV + SSM) ** -0.5, 0.125, ((1, 32),))
    return {"tokens": tokens, "documents": documents, "norm_gain": norm_gain, "out_gate_weight": out_gate_weight, "in_gate_weight": in_gate_weight, "value_weight": value_weight, "conv_taps": conv_taps, "state_in_weight": state_in_weight, "decay_rate": decay_rate, "frequency": frequency, "step_log": step_log, "input_real": input_real, "input_imag": input_imag, "readout_real": readout_real, "readout_imag": readout_imag, "skip_gain": skip_gain, "conv_out_weight": conv_out_weight, "state_out_weight": state_out_weight}


EPS = 1e-06

def pair_step(earlier, later):
    dec_real, dec_imag, sum_real, sum_imag = earlier
    late_dec_real, late_dec_imag, late_sum_real, late_sum_imag = later
    return (late_dec_real * dec_real - late_dec_imag * dec_imag, late_dec_real * dec_imag + late_dec_imag * dec_real, late_dec_real * sum_real - late_dec_imag * sum_imag + late_sum_real, late_dec_real * sum_imag + late_dec_imag * sum_real + late_sum_imag)

def ssm_constants(decay_rate, frequency, step_log, input_real, input_imag):
    step_size = jnp.exp(step_log)[:, None]
    damping = decay_rate * step_size
    turning = frequency * step_size
    fading = jnp.exp(-damping)
    coef_real = fading * jnp.cos(turning)
    coef_imag = fading * jnp.sin(turning)
    half_sine = jnp.sin(turning / 2.0)
    less_real = jnp.expm1(-damping) * jnp.cos(turning) - 2.0 * half_sine * half_sine
    denominator = decay_rate * decay_rate + frequency * frequency
    ratio_real = (-less_real * decay_rate + coef_imag * frequency) / denominator
    ratio_imag = (-coef_imag * decay_rate - less_real * frequency) / denominator
    bbar_real = ratio_real[..., None] * input_real - ratio_imag[..., None] * input_imag
    bbar_imag = ratio_real[..., None] * input_imag + ratio_imag[..., None] * input_real
    return (coef_real.reshape(-1), coef_imag.reshape(-1), bbar_real, bbar_imag)

def complex_scan(coef_real, coef_imag, bbar_real, bbar_imag, driven, keep_rows, carry_real, carry_imag, readout_real, readout_imag, block):
    groups, group_size, state_size = readout_real.shape
    row_count = driven.shape[0]
    blocks = row_count // block

    def one_block(carry, pieces):
        start_real, start_imag = carry
        inputs, keeps = pieces
        split_rows = inputs.reshape(block, groups, group_size)
        push_real = jnp.einsum('tgh,gph->tgp', split_rows, bbar_real, precision=lax.Precision.HIGHEST).reshape(block, groups * state_size)
        push_imag = jnp.einsum('tgh,gph->tgp', split_rows, bbar_imag, precision=lax.Precision.HIGHEST).reshape(block, groups * state_size)
        dec_real = coef_real[None, :] * keeps[:, None]
        dec_imag = coef_imag[None, :] * keeps[:, None]
        prod_real, prod_imag, sum_real, sum_imag = lax.associative_scan(pair_step, (dec_real, dec_imag, push_real, push_imag), axis=0)
        held_real = sum_real + prod_real * start_real[None, :] - prod_imag * start_imag[None, :]
        held_imag = sum_imag + prod_real * start_imag[None, :] + prod_imag * start_real[None, :]
        result = jnp.einsum('tgp,ghp->tgh', held_real.reshape(block, groups, state_size), readout_real, precision=lax.Precision.HIGHEST)
        result = result - jnp.einsum('tgp,ghp->tgh', held_imag.reshape(block, groups, state_size), readout_imag, precision=lax.Precision.HIGHEST)
        return ((held_real[-1], held_imag[-1]), result.reshape(block, groups * group_size))
    _, outputs = lax.scan(one_block, (carry_real, carry_imag), (driven.reshape(blocks, block, -1), keep_rows.reshape(blocks, block)))
    return outputs.reshape(row_count, groups * group_size)

def reference(tokens, documents, norm_gain, out_gate_weight, in_gate_weight, value_weight, conv_taps, state_in_weight, decay_rate, frequency, step_log, input_real, input_imag, readout_real, readout_imag, skip_gain, conv_out_weight, state_out_weight):
    values = tokens.astype(jnp.float32)
    scale = lax.rsqrt(lax.optimization_barrier(jnp.mean(values * values, axis=1, keepdims=True)) + EPS)
    normed = (values * scale * norm_gain.astype(jnp.float32)).astype(jnp.bfloat16)
    out_gate = jnp.dot(normed, out_gate_weight, preferred_element_type=jnp.float32).astype(jnp.bfloat16)
    in_gate = jnp.dot(normed, in_gate_weight, preferred_element_type=jnp.float32).astype(jnp.bfloat16)
    value = jnp.dot(normed, value_weight, preferred_element_type=jnp.float32).astype(jnp.bfloat16)
    driven = jnp.dot(normed, state_in_weight, preferred_element_type=jnp.float32).astype(jnp.bfloat16)
    product = (in_gate.astype(jnp.float32) * value.astype(jnp.float32)).astype(jnp.bfloat16)
    margin = TAPS - 1
    padded = jnp.concatenate([jnp.zeros((margin, product.shape[1]), jnp.bfloat16), product], axis=0)
    padded_docs = jnp.concatenate([jnp.full((margin,), -1, jnp.int32), documents], axis=0)
    total = jnp.zeros(product.shape, jnp.float32)
    for index in range(TAPS):
        same_doc = (padded_docs[index:index + TOKENS] == documents).astype(jnp.float32)
        total = total + conv_taps[index].astype(jnp.float32)[None, :] * padded[index:index + TOKENS].astype(jnp.float32) * same_doc[:, None]
    conv_out = (out_gate.astype(jnp.float32) * total).astype(jnp.bfloat16)
    coef_real, coef_imag, bbar_real, bbar_imag = ssm_constants(decay_rate, frequency, step_log, input_real, input_imag)
    keep_rows = jnp.concatenate([jnp.zeros((1,), jnp.float32), (documents[1:] == documents[:-1]).astype(jnp.float32)], axis=0)
    driven_wide = driven.astype(jnp.float32)
    zero_state = jnp.zeros(coef_real.shape, jnp.float32)
    readout = complex_scan(coef_real, coef_imag, bbar_real, bbar_imag, driven_wide, keep_rows, zero_state, zero_state, readout_real, readout_imag, BLOCK)
    ssm_out = jax.nn.gelu(readout + skip_gain[None, :] * driven_wide, approximate=True).astype(jnp.bfloat16)
    conv_width = CONV // N_TP
    ssm_width = SSM // N_TP
    summed = jnp.zeros((TOKENS, D), jnp.float32)
    for index in range(N_TP):
        conv_part = jnp.dot(conv_out[:, index * conv_width:(index + 1) * conv_width], conv_out_weight[index * conv_width:(index + 1) * conv_width], preferred_element_type=jnp.float32)
        ssm_part = jnp.dot(ssm_out[:, index * ssm_width:(index + 1) * ssm_width], state_out_weight[index * ssm_width:(index + 1) * ssm_width], preferred_element_type=jnp.float32)
        summed = summed + (conv_part + ssm_part).astype(jnp.bfloat16).astype(jnp.float32)
    return summed.astype(jnp.bfloat16)
```

```python
import functools

import jax
import jax.numpy as jnp
from jax import lax
from jax.experimental import pallas as pl
from jax.experimental.pallas import tpu as pltpu
from jax.sharding import PartitionSpec as P

EPS = 1e-06
LANES = 128
SUB = 8
F32 = jnp.float32
BF16 = jnp.bfloat16
SMEM = pl.BlockSpec(memory_space=pltpu.SMEM)
VMEM = pl.BlockSpec(memory_space=pltpu.VMEM)


def call(body, outs, scratch, args, name):
    return pl.pallas_call(
        body,
        out_shape=outs,
        in_specs=[SMEM] + [VMEM] * (len(args) - 1),
        out_specs=jax.tree.map(lambda _: VMEM, outs),
        scratch_shapes=scratch,
        name=name,
        compiler_params=pltpu.CompilerParams(vmem_limit_bytes=56 * 1024 * 1024),
    )(*args)


def norm_kernel(planes, ready, width, place, tokens, gain, docs, out, whole):
    if ready:
        whole[...] = tokens[...]
    else:
        values = tokens[...].astype(F32)
        scale = lax.rsqrt(jnp.sum(values * values, axis=1, keepdims=True) / width + EPS)
        whole[...] = (values * scale * gain[...].astype(F32)).astype(BF16)
    z = place[0]
    block = width // planes
    for k in range(planes):
        source = lax.rem(z - k + planes, planes) * block
        out[:, k * block : (k + 1) * block] = whole[:, pl.ds(pl.multiple_of(source, LANES), block)]
    out[:, width:] = docs[...]


def scan(steps, tiles, bu, docs, rate, start, before, keep_states):
    ar = [rate[0, :, j * LANES : (j + 1) * LANES] for j in range(tiles)]
    ai = [rate[1, :, j * LANES : (j + 1) * LANES] for j in range(tiles)]

    def one(t, carry):
        re, im, last = carry
        rows = pl.ds(pl.multiple_of(t * SUB, SUB), SUB)
        doc = docs[rows, :]
        keep = jnp.where(doc == last, 1.0, 0.0)
        new_re, new_im = [], []
        for j in range(tiles):
            r, i = keep * re[j], keep * im[j]
            lane = slice(j * LANES, (j + 1) * LANES)
            lane_im = slice((tiles + j) * LANES, (tiles + j + 1) * LANES)
            new_re.append(ar[j] * r - ai[j] * i + bu[rows, lane])
            new_im.append(ar[j] * i + ai[j] * r + bu[rows, lane_im])
            if keep_states:
                bu[rows, lane] = new_re[j]
                bu[rows, lane_im] = new_im[j]
        return new_re, new_im, doc

    return lax.fori_loop(0, steps, one, start + (before,), unroll=4)


def advance(fade_re, fade_im, alive, re, im, end_re, end_im):
    return (
        end_re + alive * (fade_re * re - fade_im * im),
        end_im + alive * (fade_re * im + fade_im * re),
    )


def wide(row, tiles):
    return jnp.concatenate([row] * tiles, axis=1)


def front_kernel(layout, place, *refs):
    planes, order, rows, width, states, steps = layout
    pieces = refs[: len(order)]
    refs = refs[len(order) :]
    weights, refs = refs[:planes], refs[planes:]
    (rate, fade, drive, u_out, gate_out, prod_out, docs_nat, ends, message) = refs[:9]
    u_nat, u_per, docs_per, bu = refs[9:]
    tiles = states // LANES
    block = width // planes
    b = place[1]
    for piece, (rel, low, size) in zip(pieces, order):
        total = jnp.dot(piece[:, :block], weights[0][...], preferred_element_type=F32)
        for k in range(1, planes):
            total = total + jnp.dot(
                piece[:, k * block : (k + 1) * block],
                weights[k][...],
                preferred_element_type=F32,
            )
        at = pl.ds(pl.multiple_of(jnp.bitwise_xor(b, rel) * rows + low, size), size)
        total = total.astype(BF16).astype(F32)
        u_nat[at, :] = total[:, :LANES]
        u_out[at, :] = total[:, :LANES].astype(BF16)
        prod_out[at, :] = (total[:, LANES : 2 * LANES] * total[:, 2 * LANES : 3 * LANES]).astype(BF16)
        gate_out[at, :] = total[:, 3 * LANES :].astype(BF16)
        docs_nat[at, :] = piece[:, width:].astype(F32)

    def permute(t, _):
        from_rows = pl.ds(t, SUB, stride=steps)
        to_rows = pl.ds(pl.multiple_of(t * SUB, SUB), SUB)
        u_per[to_rows, :] = u_nat[from_rows, :]
        docs_per[to_rows, :] = docs_nat[from_rows, :]
        return 0

    lax.fori_loop(0, steps, permute, 0, unroll=8)
    bu[...] = jnp.dot(u_per[...].astype(BF16), drive[...], preferred_element_type=F32)
    zero = [jnp.zeros((SUB, LANES), F32)] * tiles
    re, im, _ = scan(steps, tiles, bu, docs_per, rate, (zero, zero), docs_per[:SUB, :], False)
    for j in range(tiles):
        ends[0, :, j * LANES : (j + 1) * LANES] = re[j]
        ends[1, :, j * LANES : (j + 1) * LANES] = im[j]
    final = (steps - 1) * SUB
    fade_re, fade_im = fade[0, :1, :], fade[1, :1, :]
    s_re, s_im = ends[0, :1, :], ends[1, :1, :]
    for s in range(1, SUB):
        first = docs_per[s : s + 1, :]
        alive = (first == docs_per[final + s - 1 : final + s, :]) & (
            first == docs_per[final + s : final + s + 1, :]
        )
        alive = wide(jnp.where(alive, 1.0, 0.0), tiles)
        s_re, s_im = advance(
            fade_re, fade_im, alive, s_re, s_im, ends[0, s : s + 1, :], ends[1, s : s + 1, :]
        )
    message[...] = jnp.zeros_like(message)
    message[0:1, :] = s_re
    message[1:2, :] = s_im
    message[2:3, :] = wide(docs_per[:1, :], tiles)
    count = steps * SUB
    message[3:4, :] = wide(docs_per[count - 1 : count, :], tiles)
    tail = prod_out[count - 16 : count, :].astype(F32)
    message[4:6, :LANES] = tail[14:, :]
    message[6:8, :LANES] = docs_nat[count - 2 : count, :]


def back_kernel(layout, place, *refs):
    planes, members, rows, states, steps, taps_count, columns = layout
    messages, refs = refs[: planes - 1], refs[planes - 1 :]
    weights, refs = refs[:planes], refs[planes:]
    (u, gate, prod, docs_nat, ends, rate, fade, drive, readout, skip, taps) = refs[:11]
    outs = refs[11:19]
    u_nat, u_per, docs_per, bu, begin, last_docs, prod_ext, docs_ext, acts, project = refs[19:]
    tiles = states // LANES
    count = steps * SUB
    b = place[1]
    t_re = jnp.zeros((1, states), F32)
    t_im = jnp.zeros((1, states), F32)
    whole_re, whole_im = fade[2, :1, :], fade[3, :1, :]
    for k in range(planes - 1, 0, -1):
        own = messages[k - 1]
        if k < planes - 1:
            first = own[2:3, :]
            alive = (first == own[3:4, :]) & (first == messages[k][3:4, :])
            alive = jnp.where(alive, 1.0, 0.0)
        else:
            alive = jnp.zeros((1, states), F32)
        t_re, t_im = advance(whole_re, whole_im, alive, t_re, t_im, own[0:1, :], own[1:2, :])
    before = messages[0][3:4, :LANES]
    u_nat[...] = u[...].astype(F32)

    def permute(t, _):
        from_rows = pl.ds(t, SUB, stride=steps)
        to_rows = pl.ds(pl.multiple_of(t * SUB, SUB), SUB)
        u_per[to_rows, :] = u_nat[from_rows, :]
        docs_per[to_rows, :] = docs_nat[from_rows, :]
        return 0

    lax.fori_loop(0, steps, permute, 0, unroll=8)
    bu[...] = jnp.dot(u_per[...].astype(BF16), drive[...], preferred_element_type=F32)
    final = (steps - 1) * SUB
    fade_re, fade_im = fade[0, :1, :], fade[1, :1, :]
    s_re, s_im = t_re, t_im
    for s in range(SUB):
        begin[0, s : s + 1, :] = s_re
        begin[1, s : s + 1, :] = s_im
        last_docs[s : s + 1, :] = before
        first = docs_per[s : s + 1, :]
        after = docs_per[final + s : final + s + 1, :]
        alive = wide(jnp.where((first == before) & (first == after), 1.0, 0.0), tiles)
        s_re, s_im = advance(
            fade_re, fade_im, alive, s_re, s_im, ends[0, s : s + 1, :], ends[1, s : s + 1, :]
        )
        before = after
    start = tuple(
        [begin[part, :, j * LANES : (j + 1) * LANES] for j in range(tiles)] for part in range(2)
    )
    scan(steps, tiles, bu, docs_per, rate, start, last_docs[...], True)
    u_per[...] = jnp.dot(bu[...].astype(BF16), readout[...], preferred_element_type=F32)

    lax.fori_loop(0, steps, lambda t, _: _restore(t, u_per, docs_per, steps), 0, unroll=8)
    ssm = jax.nn.gelu(docs_per[...] + skip[...] * u_nat[...], approximate=True)
    acts[:, LANES:] = ssm.astype(BF16)
    prod_ext[:SUB, :] = jnp.zeros((SUB, LANES), F32)
    docs_ext[:SUB, :] = jnp.zeros((SUB, LANES), F32)
    prod_ext[6:8, :] = messages[0][4:6, :LANES]
    docs_ext[6:8, :] = messages[0][6:8, :LANES]
    prod_ext[SUB:, :] = prod[...].astype(F32)
    docs_ext[SUB:, :] = docs_nat[...]
    total = jnp.zeros((count, LANES), F32)
    for index in range(taps_count):
        at = SUB - (taps_count - 1) + index
        same = docs_ext[at : at + count, :] == docs_nat[...]
        term = taps[index : index + 1, :].astype(F32) * prod_ext[at : at + count, :]
        total = total + jnp.where(same, term, 0.0)
    acts[:, :LANES] = (gate[...].astype(F32) * total).astype(BF16)
    span = members * columns
    for k in range(planes):
        for half in range(2):
            project[half * LANES : (half + 1) * LANES, k * span : (k + 1) * span] = jnp.concatenate(
                [weights[k][m, :, half * columns : (half + 1) * columns] for m in range(members)],
                axis=1,
            )
    cut = planes * span // 2
    for rel in range(members):
        at = pl.ds(pl.multiple_of(jnp.bitwise_xor(b, rel) * rows, rows), rows)
        mine = acts[at, :]
        left = jnp.dot(mine, project[:, :cut], preferred_element_type=F32)
        right = jnp.dot(mine, project[:, cut:], preferred_element_type=F32)
        base = 4 * (rel & 1)
        x_bit, y_bit = (rel >> 1) & 1, (rel >> 2) & 1
        spot = outs[base + x_bit]
        spot[y_bit] = left.astype(spot.dtype)
        spot = outs[base + 2 + y_bit]
        spot[x_bit] = right.astype(spot.dtype)


def _restore(t, source, target, steps):
    target[pl.ds(t, SUB, stride=steps), :] = source[pl.ds(pl.multiple_of(t * SUB, SUB), SUB), :]
    return 0


def last_kernel(planes, place, left, left_in, right, right_in, out):
    z = place[0]
    cut = left.shape[1]
    block = 2 * cut // planes
    for side, (own, other) in enumerate(((left, left_in), (right, right_in))):
        for j in range(planes // 2):
            k = side * (planes // 2) + j
            target = lax.rem(z - k + planes, planes) * block
            lane = slice(j * block, (j + 1) * block)
            value = own[:, lane] + other[:, lane].astype(F32)
            out[:, pl.ds(pl.multiple_of(target, LANES), block)] = value.astype(BF16)


def ssm_constants(decay_rate, frequency, step_log, input_real, input_imag):
    step_size = jnp.exp(step_log)[:, None]
    damping = decay_rate * step_size
    turning = frequency * step_size
    fading = jnp.exp(-damping)
    coef_imag = fading * jnp.sin(turning)
    half_sine = jnp.sin(turning / 2.0)
    less_real = jnp.expm1(-damping) * jnp.cos(turning) - 2.0 * half_sine * half_sine
    denominator = decay_rate * decay_rate + frequency * frequency
    ratio_real = (-less_real * decay_rate + coef_imag * frequency) / denominator
    ratio_imag = (-coef_imag * decay_rate - less_real * frequency) / denominator
    bbar_real = ratio_real[..., None] * input_real - ratio_imag[..., None] * input_imag
    bbar_imag = ratio_real[..., None] * input_imag + ratio_imag[..., None] * input_real
    return bbar_real, bbar_imag, damping, turning


def spread(blocks, inner):
    groups, a, c = blocks.shape
    eye = jnp.eye(groups, dtype=blocks.dtype)
    return (blocks[:, :, None, :] * eye[:, None, :, None]).reshape(groups * a, groups * c)


def shards(
    planes,
    tokens,
    documents,
    norm_gain,
    out_gate_weight,
    in_gate_weight,
    value_weight,
    conv_taps,
    state_in_weight,
    decay_rate,
    frequency,
    step_log,
    input_real,
    input_imag,
    readout_real,
    readout_imag,
    skip_gain,
    conv_out_weight,
    state_out_weight,
):
    size = lax.axis_size("sp")
    parts = lax.axis_size("tp")
    members = size // planes
    place = lax.axis_index("sp")
    z, b = place // members, place % members
    where = jnp.stack([z, b]).astype(jnp.int32)
    rows = tokens.shape[0]
    width = tokens.shape[1] * parts
    count = rows * members
    steps = count // SUB
    in_rows = state_in_weight.shape[0]
    columns = conv_out_weight.shape[1]
    channels = state_in_weight.shape[1] // members
    spare = LANES - channels
    group_size = input_real.shape[2]
    groups = channels // group_size
    more = LANES // group_size - groups
    states = (groups + more) * decay_rate.shape[1]
    taps_count = conv_taps.shape[0]

    def swap(a, mask):
        return lax.ppermute(a, "sp", [(i, i ^ mask) for i in range(size)])

    def turn(a, planes_on=1):
        hop = planes_on * members
        return lax.ppermute(a, "sp", [(i, (i + hop) % size) for i in range(size)])

    def onward(a, planes_on):
        hop = planes_on * members
        return lax.ppermute(a, "sp", [(i, i + hop) for i in range(size - hop)])

    teams = [[p * members + m for m in range(members)] for p in range(planes)]

    def exchange(a):
        return lax.all_to_all(a, "sp", 0, 0, axis_index_groups=teams, tiled=True)

    def cut_in(w):
        w = w.reshape(in_rows, members, channels)
        return jnp.pad(w, ((0, 0), (0, 0), (0, spare))) if spare else w

    packed = jnp.stack(
        [cut_in(w) for w in (state_in_weight, in_gate_weight, value_weight, out_gate_weight)], axis=2
    )
    packed = packed.transpose(1, 0, 2, 3).reshape(members, in_rows, 4 * LANES)
    packed = exchange(packed).reshape(members * in_rows, 4 * LANES)
    in_blocks = [packed]
    for _ in range(planes - 1):
        in_blocks.append(turn(in_blocks[-1]))

    def cut_out(w):
        w = w.reshape(members, channels, columns)
        return jnp.pad(w, ((0, 0), (0, spare), (0, 0))) if spare else w

    outward = jnp.concatenate([cut_out(conv_out_weight), cut_out(state_out_weight)], axis=2)
    out_blocks = [exchange(outward)]
    for _ in range(planes - 1):
        out_blocks.append(turn(out_blocks[-1]))

    docs = jnp.broadcast_to(documents.astype(BF16)[:, None], (rows, LANES))
    if parts == 1:
        source = tokens
    else:
        values = tokens.astype(F32)
        totals = lax.psum(jnp.sum(values * values, axis=1), "tp")
        values = values * lax.rsqrt(totals / width + EPS)[:, None] * norm_gain.astype(F32)[None, :]
        source = lax.all_gather(values.astype(BF16), "tp", axis=1, tiled=True)
    n0 = call(
        functools.partial(norm_kernel, planes, parts > 1, width),
        jax.ShapeDtypeStruct((rows, width + LANES), BF16),
        [pltpu.VMEM((rows, width), BF16)],
        (where, source, norm_gain[None, :], docs),
        "normalize",
    )
    half = rows // 2
    n2, n4 = swap(n0, 2), swap(n0, 4)
    n1 = swap(n0, 1)
    n6 = (swap(n4[:half], 2), swap(n2[half:], 4))
    n3, n5 = swap(n2, 1), swap(n4, 1)
    n7 = (swap(n6[0], 1), swap(n6[1], 1))
    pieces = (n0, n1, n2, n4, n3, n5) + n6 + n7
    order = tuple((r, 0, rows) for r in (0, 1, 2, 4, 3, 5)) + tuple(
        (r, low, half) for r in (6, 7) for low in (0, half)
    )

    def own(a, fill=0.0):
        a = lax.dynamic_slice_in_dim(a, b * groups, groups, 0)
        if more:
            a = jnp.pad(a, ((0, more),) + ((0, 0),) * (a.ndim - 1), constant_values=fill)
        return a

    bbar_real, bbar_imag, damping, turning = ssm_constants(
        own(decay_rate, 1.0), own(frequency), own(step_log), own(input_real), own(input_imag)
    )
    damping, turning = damping.reshape(1, -1), turning.reshape(1, -1)

    def power(n):
        fading = jnp.exp(-n * damping)
        return fading * jnp.cos(n * turning), fading * jnp.sin(n * turning)

    rate = jnp.broadcast_to(jnp.stack(power(1.0)), (2, SUB, states))
    fade_re, fade_im = power(float(steps))
    whole_re, whole_im = fade_re, fade_im
    for _ in range(SUB.bit_length() - 1):
        whole_re, whole_im = whole_re * whole_re - whole_im * whole_im, 2.0 * whole_re * whole_im
    fade = jnp.broadcast_to(jnp.stack([fade_re, fade_im, whole_re, whole_im]), (4, SUB, states))
    drive = jnp.concatenate(
        [spread(m.transpose(0, 2, 1), None) for m in (bbar_real, bbar_imag)], axis=1
    ).astype(BF16)
    readout = jnp.concatenate(
        [spread(m.transpose(0, 2, 1), None) for m in (own(readout_real), -own(readout_imag))], axis=0
    ).astype(BF16)

    def own_channels(a):
        a = lax.dynamic_slice_in_dim(a, b * channels, channels, 1)
        return jnp.pad(a, ((0, 0), (0, spare))) if spare else a

    skip = own_channels(skip_gain[None, :])
    taps = own_channels(conv_taps.astype(F32))

    narrow = jax.ShapeDtypeStruct((count, LANES), BF16)
    layout = (planes, order, rows, width, states, steps)
    u, gate, prod, docs_nat, ends, message = call(
        functools.partial(front_kernel, layout),
        (
            narrow,
            narrow,
            narrow,
            jax.ShapeDtypeStruct((count, LANES), F32),
            jax.ShapeDtypeStruct((2, SUB, states), F32),
            jax.ShapeDtypeStruct((SUB, states), F32),
        ),
        [
            pltpu.VMEM((count, LANES), F32),
            pltpu.VMEM((count, LANES), F32),
            pltpu.VMEM((count, LANES), F32),
            pltpu.VMEM((count, 2 * states), F32),
        ],
        (where,) + pieces + tuple(in_blocks) + (rate, fade, drive),
        "front",
    )
    messages = tuple(onward(message, k) for k in range(1, planes))
    cut = planes * members * columns // 2
    layout = (planes, members, rows, states, steps, taps_count, columns)
    kept = jax.ShapeDtypeStruct((2, rows, cut), F32)
    sent = jax.ShapeDtypeStruct((2, rows, cut), BF16)
    outs = call(
        functools.partial(back_kernel, layout),
        (kept,) * 4 + (sent,) * 4,
        [
            pltpu.VMEM((count, LANES), F32),
            pltpu.VMEM((count, LANES), F32),
            pltpu.VMEM((count, LANES), F32),
            pltpu.VMEM((count, 2 * states), F32),
            pltpu.VMEM((2, SUB, states), F32),
            pltpu.VMEM((SUB, LANES), F32),
            pltpu.VMEM((count + SUB, LANES), F32),
            pltpu.VMEM((count + SUB, LANES), F32),
            pltpu.VMEM((count, 2 * LANES), BF16),
            pltpu.VMEM((2 * LANES, 2 * cut), BF16),
        ],
        (where,)
        + messages
        + tuple(out_blocks)
        + (u, gate, prod, docs_nat, ends, rate, fade, drive, readout, skip, taps),
        "back",
    )
    left_keep, left_send, right_keep, right_send = [
        a + swap(p, 1).astype(F32) for a, p in zip(outs[:4], outs[4:])
    ]
    left = left_keep + swap(left_send.astype(BF16), 2).astype(F32)
    right = right_keep + swap(right_send.astype(BF16), 4).astype(F32)
    left_in = swap(left[1].astype(BF16), 4)
    right_in = swap(right[1].astype(BF16), 2)
    mixed = call(
        functools.partial(last_kernel, planes),
        jax.ShapeDtypeStruct((rows, 2 * cut), BF16),
        [],
        (where, left[0], left_in, right[0], right_in),
        "finish",
    )
    if parts == 1:
        return mixed
    return lax.psum_scatter(mixed, "tp", scatter_dimension=0, tiled=True)


def solution(mesh):
    placed = (
        P(("fs", "sp"), "tp"),
        P(("fs", "sp")),
        P("tp"),
        P("sp", "tp"),
        P("sp", "tp"),
        P("sp", "tp"),
        P(None, "tp"),
        P("sp", "tp"),
        P("tp", None),
        P("tp", None),
        P("tp"),
        P("tp", None, None),
        P("tp", None, None),
        P("tp", None, None),
        P("tp", None, None),
        P("tp"),
        P("tp", "sp"),
        P("tp", "sp"),
    )
    planes = mesh.shape["sp"] // 8
    return jax.shard_map(
        functools.partial(shards, planes),
        mesh=mesh,
        in_specs=placed,
        out_specs=P(("fs", "sp", "tp"), None),
        check_vma=False,
    )
```
